32 devices in a mesh: sp: 8 (over z, x), tp: 4 (over y, core).
Axes of the slice: x: 2, y: 2, z: 4, core: 2. Of those that a mesh axis runs over, the one named last changes fastest.
Arguments:
- tokens: bfloat16 [8192, 4096], P(('sp', 'tp')), may hold values from -6 to 6
- norm_gain: float32 [4096], replicated, may hold values from 0.1 to 1.9
- q_down: bfloat16 [4096, 768], replicated, may hold values from -0.09375 to 0.09375
- kv_down: bfloat16 [4096, 512], replicated, may hold values from -0.09375 to 0.09375
- rope_down: bfloat16 [4096, 32], replicated, may hold values from -8 to 8
- q_gain: float32 [768], replicated, may hold values from 0.1 to 1.9
- kv_gain: float32 [512], replicated, may hold values from 0.1 to 1.9
- q_up: bfloat16 [768, 1536], P(None, 'tp'), may hold values from -0.21875 to 0.21875
- kv_up: bfloat16 [512, 2048], P(None, 'tp'), may hold values from -0.25 to 0.25
- out_weight: bfloat16 [1024, 4096], replicated, may hold values from -0.1875 to 0.1875
- out_gain: float32 [4096], replicated, may hold values from 0.1 to 1.9
Outputs:
- mixed: bfloat16 [8192, 4096], P(('sp', 'tp'))
The draws below stay inside these ranges and needn't reach their ends.
All inputs are finite; a program needn't handle non-finite values.
Results may differ from the reference program's by a relative error of at most 0.02.
The reference program's roundings to bfloat16 on the way (of `normed`, `q_lat`, `kv_lat`, `key_rot`, `query`, `keys_values` and `attended`) count: a program that leaves them out, or rounds other values in their place, can miss the bound.
Values may be sent and summed in bfloat16 or wider, within the bound.
A program may use at most 128 MiB of HBM per device.

```python
import jax
import jax.numpy as jnp
from jax import lax

D = 4096
HEADS = 16
NOPE = 64
ROPE = 32
VDIM = 64
Q_RANK = 768
KV_RANK = 512
TOKENS = 8192


def draw_rope_down(key, part):
    base = jax.random.normal(key, (D, ROPE), jnp.float32) * D ** (-0.5)
    return jnp.clip(base, -8.0, 8.0).astype(jnp.bfloat16)


def block_scale(stream_key, extent, split, smallest, high):
    level, own = 1.0, jax.random.fold_in(stream_key, 6)
    for dim, parts in split:
        steps = jnp.exp(jax.random.uniform(jax.random.fold_in(own, dim), (parts,), jnp.float32, smallest / len(split), high / len(split)))
        level = level * jnp.repeat(steps, extent[dim] // parts).reshape([-1 if axis == dim else 1 for axis in range(len(extent))])
    return level


def normal_values(key, dims, spread, bound, shards=(), kind=jnp.bfloat16):
    array = spread * jax.random.normal(key, dims, jnp.float32)
    if shards:
        array = array * block_scale(key, dims, shards, -0.22, 0.18)
    return jnp.clip(array, -bound, bound).astype(kind)


def setup_inputs(seed: int = 0) -> dict:
    arg_keys = jax.random.split(jax.random.key(seed), 12)
    tokens = normal_values(arg_keys[0], (TOKENS, D), 1.0, 6.0, ((0, 32),))
    norm_gain = jnp.clip(1.0 + 0.18 * jax.random.normal(arg_keys[1], (D,), jnp.float32), 0.1, 1.9)
    q_down = normal_values(arg_keys[2], (D, Q_RANK), D ** -0.5, 0.09375)
    kv_down = normal_values(arg_keys[3], (D, KV_RANK), D ** -0.5, 0.09375)
    rope_down = draw_rope_down(jax.random.fold_in(arg_keys[11], 71), 0)
    q_gain = jnp.clip(1.0 + 0.18 * jax.random.normal(arg_keys[5], (Q_RANK,), jnp.float32), 0.1, 1.9)
    kv_gain = jnp.clip(1.0 + 0.18 * jax.random.normal(arg_keys[6], (KV_RANK,), jnp.float32), 0.1, 1.9)
    q_up = normal_values(arg_keys[7], (Q_RANK, HEADS * (NOPE + ROPE)), Q_RANK ** -0.5, 0.21875, ((1, 4),))
    kv_up = normal_values(arg_keys[8], (KV_RANK, HEADS * (NOPE + VDIM)), KV_RANK ** -0.5, 0.25, ((1, 4),))
    out_weight = normal_values(arg_keys[9], (HEADS * VDIM, D), (HEADS * VDIM) ** -0.5, 0.1875)
    out_gain = jnp.clip(1.0 + 0.18 * jax.random.normal(arg_keys[10], (D,), jnp.float32), 0.1, 1.9)
    return dict(tokens=tokens, norm_gain=norm_gain, q_down=q_down, kv_down=kv_down, rope_down=rope_down, q_gain=q_gain, kv_gain=kv_gain, q_up=q_up, kv_up=kv_up, out_weight=out_weight, out_gain=out_gain)


EPS = 1e-06
THETA = 500000.0

def scaled_norm(values_in, gain):
    values_in = values_in.astype(jnp.float32)
    return values_in * lax.rsqrt(lax.optimization_barrier(jnp.mean(values_in * values_in, axis=-1, keepdims=True)) + EPS) * gain.astype(jnp.float32)

def rotate(values_in, position):
    values_in = values_in.astype(jnp.float32)
    width = values_in.shape[-1]
    half_dim = width // 2
    inverse = 1.0 / THETA ** (jnp.arange(0, width, 2, dtype=jnp.float32) / width)
    angles = position[:, None] * inverse[None, :]
    angles = angles.reshape((angles.shape[0],) + (1,) * (values_in.ndim - 2) + (half_dim,))
    cosine = jnp.cos(angles)
    sine = jnp.sin(angles)
    left = values_in[..., :half_dim]
    right = values_in[..., half_dim:]
    return jnp.concatenate([left * cosine - right * sine, right * cosine + left * sine], axis=-1)

def reference(tokens, norm_gain, q_down, kv_down, rope_down, q_gain, kv_gain, q_up, kv_up, out_weight, out_gain):
    position = jnp.arange(TOKENS, dtype=jnp.float32)
    normed = scaled_norm(tokens, norm_gain).astype(jnp.bfloat16)
    q_lat = scaled_norm(jnp.dot(normed, q_down, preferred_element_type=jnp.float32), q_gain).astype(jnp.bfloat16)
    kv_lat = scaled_norm(jnp.dot(normed, kv_down, preferred_element_type=jnp.float32), kv_gain).astype(jnp.bfloat16)
    key_rot = rotate(jnp.dot(normed, rope_down, preferred_element_type=jnp.float32), position).astype(jnp.bfloat16)
    query = jnp.dot(q_lat, q_up, preferred_element_type=jnp.float32).reshape(TOKENS, HEADS, NOPE + ROPE)
    query = jnp.concatenate([query[..., :NOPE], rotate(query[..., NOPE:], position)], axis=-1).astype(jnp.bfloat16)
    keys_values = jnp.dot(kv_lat, kv_up, preferred_element_type=jnp.float32).astype(jnp.bfloat16)
    keys_values = keys_values.reshape(TOKENS, HEADS, NOPE + VDIM)
    key_nope = keys_values[..., :NOPE].astype(jnp.float32)
    values = keys_values[..., NOPE:].astype(jnp.float32)
    key_rot32 = key_rot.astype(jnp.float32)
    factor = (NOPE + ROPE) ** (-0.5)
    block_rows = 256 if TOKENS % 256 == 0 else TOKENS
    key_index = jnp.arange(TOKENS)

    def attend(index):
        first_row = index * block_rows
        query_block = lax.dynamic_slice_in_dim(query, first_row, block_rows, 0).astype(jnp.float32)
        scores = jnp.einsum('qhd,khd->hqk', query_block[..., :NOPE], key_nope)
        scores = (scores + jnp.einsum('qhd,kd->hqk', query_block[..., NOPE:], key_rot32)) * factor
        query_index = first_row + jnp.arange(block_rows)
        visible = key_index[None, :] <= query_index[:, None]
        scores = jnp.where(visible[None], scores, -1e+30)
        top_score = lax.optimization_barrier(jnp.max(scores, axis=-1, keepdims=True))
        weights = jnp.where(visible[None], jnp.exp(scores - top_score), 0.0)
        total = lax.optimization_barrier(jnp.sum(weights, axis=-1))
        rounded = lax.optimization_barrier(weights.astype(jnp.bfloat16)).astype(jnp.float32)
        summed = jnp.einsum('hqk,khd->qhd', rounded, values)
        return (summed / total.T[:, :, None]).astype(jnp.bfloat16)
    attended = lax.map(attend, jnp.arange(TOKENS // block_rows)).reshape(TOKENS, HEADS * VDIM)
    projected = jnp.dot(attended, out_weight, preferred_element_type=jnp.float32)
    return scaled_norm(projected, out_gain).astype(jnp.bfloat16)
```

```python
import functools

import jax
import jax.numpy as jnp
from jax import lax
from jax.experimental import pallas as pl
from jax.experimental.pallas import tpu as pltpu
from jax.sharding import PartitionSpec as P

NOPE = 64
ROPE = 32
VDIM = 64
HEAD_KV = NOPE + VDIM

EPS = 1e-06
THETA = 500000.0
LOG2E = 1.4426950408889634
FLOOR = -1e30
Q_TILE = 256
K_TILE = 512
V_ROWS = VDIM + 16


def scaled_norm(values_in, gain):
    values_in = values_in.astype(jnp.float32)
    return (
        values_in * lax.rsqrt(jnp.mean(values_in * values_in, axis=-1, keepdims=True) + EPS) * gain
    )


def angle_tables(position):
    inverse = 1.0 / THETA ** (jnp.arange(0, ROPE, 2, dtype=jnp.float32) / ROPE)
    return position.astype(jnp.float32)[:, None] * inverse[None, :]


def rotate(values_in, position):
    angles = angle_tables(position)
    cosine = jnp.cos(angles)
    sine = jnp.sin(angles)
    left = values_in[:, : ROPE // 2]
    right = values_in[:, ROPE // 2 :]
    return jnp.concatenate([left * cosine - right * sine, right * cosine + left * sine], axis=-1)


def attend_kernel(
    rows,
    heads,
    group_rows,
    rank,
    place_ref,
    q_lat_ref,
    q_up_ref,
    cos_ref,
    sin_ref,
    position_ref,
    lat_ref,
    kv_up_ref,
    v_up_ref,
    out_ref,
    query_ref,
    key_ref,
    value_ref,
    sum_ref,
    top_ref,
):
    chunk = pl.program_id(0)
    half = rows // 2
    side = group_rows // 2
    width = NOPE + ROPE
    scale = width**-0.5 * LOG2E

    @pl.when(chunk == 0)
    def _():
        cosine = cos_ref[...]
        sine = sin_ref[...]
        middle = NOPE + ROPE // 2
        for head in range(heads):
            turned = lax.dot_general(
                q_up_ref[head],
                q_lat_ref[...],
                (((1,), (1,)), ((), ())),
                preferred_element_type=jnp.float32,
            )
            left = turned[NOPE:middle]
            right = turned[middle:]
            query_ref[head, :NOPE] = turned[:NOPE].astype(jnp.bfloat16)
            query_ref[head, NOPE:middle] = (left * cosine - right * sine).astype(jnp.bfloat16)
            query_ref[head, middle:width] = (right * cosine + left * sine).astype(jnp.bfloat16)
            query_ref[head, width:] = jnp.zeros((128 - width, group_rows), jnp.bfloat16)
            row = lax.broadcasted_iota(jnp.int32, (16, group_rows), 0)
            value_ref[head, VDIM:] = jnp.where(row == 0, 1.0, 0.0).astype(jnp.bfloat16)
            sum_ref[head] = jnp.zeros((V_ROWS, group_rows), jnp.float32)
            top_ref[head] = jnp.full((1, group_rows), FLOOR, jnp.float32)

    own = place_ref[0]
    mate = place_ref[1]

    @pl.when(chunk <= jnp.maximum(own, mate))
    def _():
        lat = lat_ref[:, :rank]
        turned = lat_ref[:, rank:]
        lane = lax.broadcasted_iota(jnp.int32, (group_rows, HEAD_KV), 1)
        for head in range(heads):
            raw = jnp.dot(
                lat,
                kv_up_ref[:, head * HEAD_KV : (head + 1) * HEAD_KV],
                preferred_element_type=jnp.float32,
            ).astype(jnp.bfloat16)
            key_ref[head] = jnp.where(lane < NOPE, raw, turned)
        values = lax.dot_general(
            v_up_ref[...], lat, (((1,), (1,)), ((), ())), preferred_element_type=jnp.float32
        ).astype(jnp.bfloat16)
        for head in range(heads):
            value_ref[head, :VDIM] = values[head * VDIM : (head + 1) * VDIM]

        key_steps = group_rows // K_TILE
        query_steps = group_rows // Q_TILE

        def pair(masked, column, key_row):
            columns = pl.ds(column, Q_TILE)
            keys = pl.ds(key_row, K_TILE)
            if masked:
                key_index = (
                    chunk * group_rows
                    + key_row
                    + lax.broadcasted_iota(jnp.int32, (K_TILE, Q_TILE), 0)
                )
                visible = key_index <= position_ref[:, columns]
            for head in range(heads):
                scores = jnp.dot(
                    key_ref[head, keys, :],
                    query_ref[head, :, columns],
                    preferred_element_type=jnp.float32,
                )
                if masked:
                    scores = jnp.where(visible, scores, FLOOR)
                old = top_ref[head, :, columns]
                new = jnp.maximum(old, jnp.max(scores, axis=0, keepdims=True))
                weights = jnp.exp2((scores - new) * scale)
                product = jnp.dot(
                    value_ref[head, :, keys],
                    weights.astype(jnp.bfloat16),
                    preferred_element_type=jnp.float32,
                )
                sum_ref[head, :, columns] = (
                    sum_ref[head, :, columns] * jnp.exp2((old - new) * scale) + product
                )
                top_ref[head, :, columns] = new

        @pl.loop(0, key_steps * query_steps)
        def _(index):
            column = pl.multiple_of(lax.rem(index, query_steps) * Q_TILE, Q_TILE)
            key_row = pl.multiple_of(lax.div(index, query_steps) * K_TILE, K_TILE)
            second = column >= side
            group = jnp.where(second, mate, own)
            inside = column - jnp.where(second, side, 0)
            base = group * group_rows + jnp.where(second, half, 0)
            first_query = base + lax.div(inside, half) * rows + lax.rem(inside, half)
            last = inside + Q_TILE - 1
            last_query = base + lax.div(last, half) * rows + lax.rem(last, half)
            first_key = chunk * group_rows + key_row
            last_key = first_key + K_TILE - 1

            @pl.when(last_key <= first_query)
            def _():
                pair(False, column, key_row)

            @pl.when((last_key > first_query) & (first_key <= last_query))
            def _():
                pair(True, column, key_row)

    @pl.when(chunk == pl.num_programs(0) - 1)
    def _():
        for column in range(0, group_rows, Q_TILE):
            columns = slice(column, column + Q_TILE)
            parts = [
                sum_ref[head, :VDIM, columns] / sum_ref[head, VDIM : VDIM + 1, columns]
                for head in range(heads)
            ]
            out_ref[columns, :] = jnp.concatenate(parts, axis=0).T.astype(jnp.bfloat16)


def attend(place, q_lat, q_up, cosine, sine, position, latents, kv_up, v_up, rows):
    group_rows, q_rank = q_lat.shape
    heads = q_up.shape[0]
    rank = kv_up.shape[0]
    chunks = latents.shape[0] // group_rows

    def whole(*shape):
        return pl.BlockSpec(shape, lambda chunk, place_ref: (0,) * len(shape))

    pairs = latents.shape[0] * group_rows * heads // 2
    return pl.pallas_call(
        functools.partial(attend_kernel, rows, heads, group_rows, rank),
        out_shape=jax.ShapeDtypeStruct((group_rows, heads * VDIM), jnp.bfloat16),
        grid_spec=pltpu.PrefetchScalarGridSpec(
            num_scalar_prefetch=1,
            grid=(chunks,),
            in_specs=[
                whole(group_rows, q_rank),
                whole(heads, NOPE + ROPE, q_rank),
                whole(ROPE // 2, group_rows),
                whole(ROPE // 2, group_rows),
                whole(1, group_rows),
                pl.BlockSpec(
                    (group_rows, latents.shape[1]),
                    lambda chunk, place_ref: (
                        jnp.minimum(chunk, jnp.maximum(place_ref[0], place_ref[1])),
                        0,
                    ),
                ),
                whole(*kv_up.shape),
                whole(*v_up.shape),
            ],
            out_specs=whole(group_rows, heads * VDIM),
            scratch_shapes=[
                pltpu.VMEM((heads, 128, group_rows), jnp.bfloat16),
                pltpu.VMEM((heads, group_rows, HEAD_KV), jnp.bfloat16),
                pltpu.VMEM((heads, V_ROWS, group_rows), jnp.bfloat16),
                pltpu.VMEM((heads, V_ROWS, group_rows), jnp.float32),
                pltpu.VMEM((heads, 1, group_rows), jnp.float32),
            ],
        ),
        compiler_params=pltpu.CompilerParams(
            dimension_semantics=("arbitrary",), vmem_limit_bytes=48 * 1024 * 1024
        ),
        cost_estimate=pl.CostEstimate(
            flops=pairs * 640, bytes_accessed=latents.size * 2, transcendentals=pairs
        ),
    )(place, q_lat, q_up, cosine, sine, position, latents, kv_up, v_up)


def local(
    tokens,
    norm_gain,
    q_down,
    kv_down,
    rope_down,
    q_gain,
    kv_gain,
    q_up,
    kv_up,
    out_weight,
    out_gain,
):
    rows = tokens.shape[0]
    tp_count = lax.axis_size("tp")
    sp_count = lax.axis_size("sp")
    tp_place = lax.axis_index("tp")
    sp_place = lax.axis_index("sp")
    group_rows = rows * tp_count
    half = rows // 2
    row_first = (sp_place * tp_count + tp_place) * rows
    own_position = row_first + jnp.arange(rows)
    heads = q_up.shape[1] // (NOPE + ROPE)
    rank = kv_up.shape[0]

    normed = scaled_norm(tokens, norm_gain).astype(jnp.bfloat16)
    kv_lat = scaled_norm(
        jnp.dot(normed, kv_down, preferred_element_type=jnp.float32), kv_gain
    ).astype(jnp.bfloat16)
    key_rot = rotate(
        jnp.dot(normed, rope_down, preferred_element_type=jnp.float32), own_position
    ).astype(jnp.bfloat16)
    packed = jnp.concatenate(
        [
            kv_lat,
            jnp.zeros((rows, NOPE), jnp.bfloat16),
            key_rot,
            jnp.zeros((rows, 128 - NOPE - ROPE), jnp.bfloat16),
        ],
        axis=1,
    )
    latents = lax.all_gather(packed, ("sp", "tp"), axis=0, tiled=True)

    q_lat = scaled_norm(jnp.dot(normed, q_down, preferred_element_type=jnp.float32), q_gain).astype(
        jnp.bfloat16
    )
    swap = [(place, sp_count - 1 - place) for place in range(sp_count)]
    other = lax.ppermute(q_lat[half:], "sp", swap)
    q_pair = jnp.concatenate([q_lat[:half], other], axis=0)
    q_group = lax.all_gather(q_pair, "tp", axis=0, tiled=True)
    q_group = (
        q_group.reshape(tp_count, 2, half, -1).transpose(1, 0, 2, 3).reshape(group_rows, -1)
    )
    mate = sp_count - 1 - sp_place
    base = jnp.stack([sp_place * group_rows, mate * group_rows + half])
    position = (
        base[:, None, None]
        + (jnp.arange(tp_count) * rows)[None, :, None]
        + jnp.arange(half)[None, None, :]
    ).reshape(group_rows)
    angles = angle_tables(position).T

    q_up_turned = q_up.reshape(-1, heads, NOPE + ROPE).transpose(1, 2, 0)
    v_up = kv_up.reshape(rank, heads, HEAD_KV)[:, :, NOPE:].transpose(1, 2, 0)
    attended = attend(
        jnp.stack([sp_place, mate]).astype(jnp.int32),
        q_group,
        q_up_turned,
        jnp.cos(angles),
        jnp.sin(angles),
        position.astype(jnp.int32)[None, :],
        latents,
        kv_up,
        v_up.reshape(heads * VDIM, rank),
        rows,
    )
    own_heads = lax.all_to_all(
        attended.reshape(2, tp_count, half, heads * VDIM),
        "tp",
        split_axis=1,
        concat_axis=3,
        tiled=True,
    )
    returned = lax.ppermute(own_heads[1, 0], "sp", swap)
    own_rows = jnp.concatenate([own_heads[0, 0], returned], axis=0)
    projected = jnp.dot(own_rows, out_weight, preferred_element_type=jnp.float32)
    return scaled_norm(projected, out_gain).astype(jnp.bfloat16)


def solution(mesh):
    return jax.shard_map(
        local,
        mesh=mesh,
        in_specs=(
            P(("sp", "tp"), None),
            P(),
            P(),
            P(),
            P(),
            P(),
            P(),
            P(None, "tp"),
            P(None, "tp"),
            P(),
            P(),
        ),
        out_specs=P(("sp", "tp"), None),
        check_vma=False,
    )
```

```python
import functools

import jax
import jax.numpy as jnp
from jax import lax
from jax.experimental import pallas as pl
from jax.experimental.pallas import tpu as pltpu
from jax.sharding import PartitionSpec as P

NOPE = 64
ROPE = 32
VDIM = 64
HEAD_KV = NOPE + VDIM

EPS = 1e-06
THETA = 500000.0
LOG2E = 1.4426950408889634
FLOOR = -1e30
Q_TILE = 256
K_TILE = 512
V_ROWS = VDIM + 16


def scaled_norm(values_in, gain):
    values_in = values_in.astype(jnp.float32)
    return (
        values_in * lax.rsqrt(jnp.mean(values_in * values_in, axis=-1, keepdims=True) + EPS) * gain
    )


def angle_tables(position):
    inverse = 1.0 / THETA ** (jnp.arange(0, ROPE, 2, dtype=jnp.float32) / ROPE)
    return position.astype(jnp.float32)[:, None] * inverse[None, :]


def rotate(values_in, position):
    angles = angle_tables(position)
    cosine = jnp.cos(angles)
    sine = jnp.sin(angles)
    left = values_in[:, : ROPE // 2]
    right = values_in[:, ROPE // 2 :]
    return jnp.concatenate([left * cosine - right * sine, right * cosine + left * sine], axis=-1)


def attend_kernel(
    rows,
    heads,
    group_rows,
    rank,
    place_ref,
    q_lat_ref,
    q_up_ref,
    cos_ref,
    sin_ref,
    position_ref,
    lat_ref,
    kv_up_ref,
    v_up_ref,
    out_ref,
    query_ref,
    key_ref,
    value_ref,
    sum_ref,
    top_ref,
):
    chunk = pl.program_id(0)
    half = rows // 2
    side = group_rows // 2
    width = NOPE + ROPE
    scale = width**-0.5 * LOG2E

    @pl.when(chunk == 0)
    def _():
        cosine = cos_ref[...]
        sine = sin_ref[...]
        middle = NOPE + ROPE // 2
        for head in range(heads):
            turned = lax.dot_general(
                q_up_ref[head],
                q_lat_ref[...],
                (((1,), (1,)), ((), ())),
                preferred_element_type=jnp.float32,
            )
            left = turned[NOPE:middle]
            right = turned[middle:]
            query_ref[head, :NOPE] = turned[:NOPE].astype(jnp.bfloat16)
            query_ref[head, NOPE:middle] = (left * cosine - right * sine).astype(jnp.bfloat16)
            query_ref[head, middle:width] = (right * cosine + left * sine).astype(jnp.bfloat16)
            query_ref[head, width:] = jnp.zeros((128 - width, group_rows), jnp.bfloat16)
            row = lax.broadcasted_iota(jnp.int32, (16, group_rows), 0)
            value_ref[head, VDIM:] = jnp.where(row == 0, 1.0, 0.0).astype(jnp.bfloat16)
            sum_ref[head] = jnp.zeros((V_ROWS, group_rows), jnp.float32)
            top_ref[head] = jnp.full((1, group_rows), FLOOR, jnp.float32)

    own = place_ref[0]
    mate = place_ref[1]

    @pl.when(chunk <= jnp.maximum(own, mate))
    def _():
        lat = lat_ref[:, :rank]
        turned = lat_ref[:, rank:]
        lane = lax.broadcasted_iota(jnp.int32, (group_rows, HEAD_KV), 1)
        for head in range(heads):
            raw = jnp.dot(
                lat,
                kv_up_ref[:, head * HEAD_KV : (head + 1) * HEAD_KV],
                preferred_element_type=jnp.float32,
            ).astype(jnp.bfloat16)
            key_ref[head] = jnp.where(lane < NOPE, raw, turned)
        values = lax.dot_general(
            v_up_ref[...], lat, (((1,), (1,)), ((), ())), preferred_element_type=jnp.float32
        ).astype(jnp.bfloat16)
        for head in range(heads):
            value_ref[head, :VDIM] = values[head * VDIM : (head + 1) * VDIM]

        key_steps = group_rows // K_TILE
        query_steps = group_rows // Q_TILE

        def pair(masked, column, key_row):
            columns = pl.ds(column, Q_TILE)
            keys = pl.ds(key_row, K_TILE)
            if masked:
                key_index = (
                    chunk * group_rows
                    + key_row
                    + lax.broadcasted_iota(jnp.int32, (K_TILE, Q_TILE), 0)
                )
                visible = key_index <= position_ref[:, columns]
            for head in range(heads):
                scores = jnp.dot(
                    key_ref[head, keys, :],
                    query_ref[head, :, columns],
                    preferred_element_type=jnp.float32,
                )
                if masked:
                    scores = jnp.where(visible, scores, FLOOR)
                old = top_ref[head, :, columns]
                new = jnp.maximum(old, jnp.max(scores, axis=0, keepdims=True))
                weights = jnp.exp2((scores - new) * scale)
                product = jnp.dot(
                    value_ref[head, :, keys],
                    weights.astype(jnp.bfloat16),
                    preferred_element_type=jnp.float32,
                )
                sum_ref[head, :, columns] = (
                    sum_ref[head, :, columns] * jnp.exp2((old - new) * scale) + product
                )
                top_ref[head, :, columns] = new

        @pl.loop(0, key_steps * query_steps)
        def _(index):
            column = pl.multiple_of(lax.rem(index, query_steps) * Q_TILE, Q_TILE)
            key_row = pl.multiple_of(lax.div(index, query_steps) * K_TILE, K_TILE)
            second = column >= side
            group = jnp.where(second, mate, own)
            inside = column - jnp.where(second, side, 0)
            base = group * group_rows + jnp.where(second, half, 0)
            first_query = base + lax.div(inside, half) * rows + lax.rem(inside, half)
            last = inside + Q_TILE - 1
            last_query = base + lax.div(last, half) * rows + lax.rem(last, half)
            first_key = chunk * group_rows + key_row
            last_key = first_key + K_TILE - 1

            @pl.when(last_key <= first_query)
            def _():
                pair(False, column, key_row)

            @pl.when((last_key > first_query) & (first_key <= last_query))
            def _():
                pair(True, column, key_row)

    @pl.when(chunk == pl.num_programs(0) - 1)
    def _():
        for column in range(0, group_rows, Q_TILE):
            columns = slice(column, column + Q_TILE)
            parts = [
                sum_ref[head, :VDIM, columns] / sum_ref[head, VDIM : VDIM + 1, columns]
                for head in range(heads)
            ]
            out_ref[columns, :] = jnp.concatenate(parts, axis=0).T.astype(jnp.bfloat16)


def attend(place, q_lat, q_up, cosine, sine, position, latents, kv_up, v_up, rows):
    group_rows, q_rank = q_lat.shape
    heads = q_up.shape[0]
    rank = kv_up.shape[0]
    chunks = latents.shape[0] // group_rows

    def whole(*shape):
        return pl.BlockSpec(shape, lambda chunk, place_ref: (0,) * len(shape))

    pairs = latents.shape[0] * group_rows * heads // 2
    return pl.pallas_call(
        functools.partial(attend_kernel, rows, heads, group_rows, rank),
        out_shape=jax.ShapeDtypeStruct((group_rows, heads * VDIM), jnp.bfloat16),
        grid_spec=pltpu.PrefetchScalarGridSpec(
            num_scalar_prefetch=1,
            grid=(chunks,),
            in_specs=[
                whole(group_rows, q_rank),
                whole(heads, NOPE + ROPE, q_rank),
                whole(ROPE // 2, group_rows),
                whole(ROPE // 2, group_rows),
                whole(1, group_rows),
                pl.BlockSpec(
                    (group_rows, latents.shape[1]),
                    lambda chunk, place_ref: (
                        jnp.minimum(chunk, jnp.maximum(place_ref[0], place_ref[1])),
                        0,
                    ),
                ),
                whole(*kv_up.shape),
                whole(*v_up.shape),
            ],
            out_specs=whole(group_rows, heads * VDIM),
            scratch_shapes=[
                pltpu.VMEM((heads, 128, group_rows), jnp.bfloat16),
                pltpu.VMEM((heads, group_rows, HEAD_KV), jnp.bfloat16),
                pltpu.VMEM((heads, V_ROWS, group_rows), jnp.bfloat16),
                pltpu.VMEM((heads, V_ROWS, group_rows), jnp.float32),
                pltpu.VMEM((heads, 1, group_rows), jnp.float32),
            ],
        ),
        compiler_params=pltpu.CompilerParams(
            dimension_semantics=("arbitrary",), vmem_limit_bytes=48 * 1024 * 1024
        ),
        cost_estimate=pl.CostEstimate(
            flops=pairs * 640, bytes_accessed=latents.size * 2, transcendentals=pairs
        ),
    )(place, q_lat, q_up, cosine, sine, position, latents, kv_up, v_up)


def plane_place(x, y, x_count, y_count):
    down = y_count - 1 - y
    across = jnp.where(lax.rem(down, 2) == 0, x - 1, x_count - 1 - x)
    return jnp.where(x == 0, y, y_count + down * (x_count - 1) + across)


def plane_chip(place, x_count, y_count):
    rest = jnp.maximum(place - y_count, 0)
    down = lax.div(rest, x_count - 1)
    step = lax.rem(rest, x_count - 1)
    across = jnp.where(lax.rem(down, 2) == 0, 1 + step, x_count - 1 - step)
    first = place < y_count
    return jnp.where(first, 0, across), jnp.where(first, place, y_count - 1 - down)


def ring_offsets(count):
    order = [0]
    for distance in range(1, count // 2 + 1):
        order.append(distance)
        if distance < count - distance:
            order.append(-distance)
    return order


def gather_kernel(
    sp_count, tp_count, lat_ref, q_ref, all_ref, q_all_ref, send_sem, recv_sem, q_send, q_recv, own_sem
):
    rows = lat_ref.shape[0]
    half = rows // 2
    y_count = tp_count // 2
    x_count = y_count
    z_count = sp_count // x_count
    plane_count = x_count * y_count
    sp = lax.axis_index("sp")
    tp = lax.axis_index("tp")
    z, x = lax.div(sp, x_count), lax.rem(sp, x_count)
    y, core = lax.div(tp, 2), lax.rem(tp, 2)
    plane = plane_place(x, y, x_count, y_count)
    mate = sp_count - 1 - sp

    def device(z_at, plane_at, core_at):
        x_at, y_at = plane_chip(plane_at, x_count, y_count)
        return z_at * x_count + x_at, y_at * 2 + core_at

    def wrap(value, count):
        return lax.rem(value + count, count)

    z_up, z_down = wrap(z + 1, z_count), wrap(z - 1, z_count)
    p_up, p_down = wrap(plane + 1, plane_count), wrap(plane - 1, plane_count)
    neighbours = [
        device(z_up, plane, core),
        device(z_down, plane, core),
        device(z, p_up, core),
        device(z, p_down, core),
    ]
    others = [wrap(tp + step, tp_count) for step in range(1, tp_count)]
    greeted = neighbours + [(sp, other) for other in others]
    greeted += [(mate, wrap(tp + step, tp_count)) for step in range(tp_count)]
    barrier = pltpu.get_barrier_semaphore()
    for target in greeted:
        pl.semaphore_signal(
            barrier, inc=1, device_id=target, device_id_type=pl.DeviceIdType.MESH
        )
    pl.semaphore_wait(barrier, len(greeted))

    own_slot = sp * tp_count + tp
    own_copies = [
        pltpu.make_async_copy(lat_ref, all_ref.at[own_slot], own_sem.at[0]),
        pltpu.make_async_copy(q_ref.at[pl.ds(0, half)], q_all_ref.at[0, tp], own_sem.at[1]),
    ]
    for copy in own_copies:
        copy.start()

    def q_copy(side, target, index):
        return pltpu.make_async_remote_copy(
            src_ref=q_ref.at[pl.ds(side * half, half)],
            dst_ref=q_all_ref.at[side, tp],
            send_sem=q_send.at[index],
            recv_sem=q_recv.at[side, tp],
            device_id=target,
            device_id_type=pl.DeviceIdType.MESH,
        )

    q_copies = [q_copy(0, (sp, other), index) for index, other in enumerate(others)]
    q_copies += [
        q_copy(1, (mate, wrap(tp + step, tp_count)), tp_count - 1 + step)
        for step in range(tp_count)
    ]

    def spread(core_at, count_1, count_2, at_1, at_2, place):
        sent = []

        def part(slot, piece):
            return all_ref.at[slot, pl.ds(piece * half, half)]

        def slot_of(one, two, core_of):
            sp_of, tp_of = device(*place(one, two), core_of)
            return sp_of * tp_count + tp_of

        def push(slot, piece, target, mine):
            source = lat_ref.at[pl.ds(piece * half, half)] if mine else part(slot, piece)
            copy = pltpu.make_async_remote_copy(
                src_ref=source,
                dst_ref=part(slot, piece),
                send_sem=send_sem.at[len(sent)],
                recv_sem=recv_sem.at[slot, piece],
                device_id=target,
                device_id_type=pl.DeviceIdType.MESH,
            )
            copy.start()
            sent.append(copy)

        def arrive(slot, piece):
            pltpu.make_async_remote_copy(
                src_ref=part(slot, piece),
                dst_ref=part(slot, piece),
                send_sem=send_sem.at[0],
                recv_sem=recv_sem.at[slot, piece],
                device_id=neighbours[0],
                device_id_type=pl.DeviceIdType.MESH,
            ).wait_recv()

        def onward(slot, offset, piece, count, up, down, mine):
            far = count // 2
            if offset <= 0 and offset != far:
                distance = 1 - offset
                if distance < far or (distance == far and piece == 1):
                    push(slot, piece, down, mine)
            if offset >= 0 and offset != far:
                distance = 1 + offset
                if distance < far or (distance == far and piece == 0):
                    push(slot, piece, up, mine)

        up_1 = device(*place(wrap(at_1 + 1, count_1), at_2), core_at)
        down_1 = device(*place(wrap(at_1 - 1, count_1), at_2), core_at)
        up_2 = device(*place(at_1, wrap(at_2 + 1, count_2)), core_at)
        down_2 = device(*place(at_1, wrap(at_2 - 1, count_2)), core_at)
        partner = (sp, y * 2 + 1 - core_at)
        items = [(one, two) for one in ring_offsets(count_1) for two in ring_offsets(count_2)]
        items.sort(key=lambda item: (abs(item[0]) + abs(item[1]), abs(item[1])))
        for one, two in items:
            slot = slot_of(wrap(at_1 - one, count_1), wrap(at_2 - two, count_2), core_at)
            mine = one == 0 and two == 0
            for piece in range(2):
                if not mine:
                    arrive(slot, piece)
                if two == 0:
                    onward(slot, one, piece, count_1, up_1, down_1, mine)
                onward(slot, two, piece, count_2, up_2, down_2, mine)
                push(slot, piece, partner, mine)
            if mine:
                for copy in q_copies:
                    copy.start()
        for one, two in items:
            slot = slot_of(wrap(at_1 - one, count_1), wrap(at_2 - two, count_2), 1 - core_at)
            for piece in range(2):
                arrive(slot, piece)
        for copy in sent:
            copy.wait_send()

    @pl.when(core == 0)
    def _():
        spread(0, plane_count, z_count, plane, z, lambda one, two: (two, one))

    @pl.when(core == 1)
    def _():
        spread(1, z_count, plane_count, z, plane, lambda one, two: (one, two))

    for index, copy in enumerate(q_copies):
        copy.wait_send()
    for side, source in [(0, other) for other in others] + [(1, at) for at in range(tp_count)]:
        pltpu.make_async_remote_copy(
            src_ref=q_all_ref.at[side, source],
            dst_ref=q_all_ref.at[side, source],
            send_sem=q_send.at[0],
            recv_sem=q_recv.at[side, source],
            device_id=neighbours[0],
            device_id_type=pl.DeviceIdType.MESH,
        ).wait_recv()
    for copy in own_copies:
        copy.wait()


def gather(latents, q_lat):
    sp_count = lax.axis_size("sp")
    tp_count = lax.axis_size("tp")
    rows, width = latents.shape
    count = sp_count * tp_count
    space = pl.BlockSpec(memory_space=pltpu.VMEM)
    everywhere, q_all = pl.pallas_call(
        functools.partial(gather_kernel, sp_count, tp_count),
        out_shape=(
            jax.ShapeDtypeStruct((count, rows, width), latents.dtype),
            jax.ShapeDtypeStruct((2, tp_count, rows // 2, q_lat.shape[1]), q_lat.dtype),
        ),
        in_specs=[space, space],
        out_specs=(pl.BlockSpec(memory_space=pl.ANY), pl.BlockSpec(memory_space=pl.ANY)),
        scratch_shapes=[
            pltpu.SemaphoreType.DMA((4 * count,)),
            pltpu.SemaphoreType.DMA((count, 2)),
            pltpu.SemaphoreType.DMA((2 * tp_count,)),
            pltpu.SemaphoreType.DMA((2, tp_count)),
            pltpu.SemaphoreType.DMA((2,)),
        ],
        compiler_params=pltpu.CompilerParams(collective_id=0, has_side_effects=True),
        cost_estimate=pl.CostEstimate(
            flops=0, bytes_accessed=count * rows * width * 8, transcendentals=0
        ),
    )(latents, q_lat)
    return everywhere.reshape(count * rows, width), q_all.reshape(tp_count * rows, -1)


def local(
    tokens,
    norm_gain,
    q_down,
    kv_down,
    rope_down,
    q_gain,
    kv_gain,
    q_up,
    kv_up,
    out_weight,
    out_gain,
):
    rows = tokens.shape[0]
    tp_count = lax.axis_size("tp")
    sp_count = lax.axis_size("sp")
    tp_place = lax.axis_index("tp")
    sp_place = lax.axis_index("sp")
    group_rows = rows * tp_count
    half = rows // 2
    row_first = (sp_place * tp_count + tp_place) * rows
    own_position = row_first + jnp.arange(rows)
    heads = q_up.shape[1] // (NOPE + ROPE)
    rank = kv_up.shape[0]

    normed = scaled_norm(tokens, norm_gain).astype(jnp.bfloat16)
    kv_lat = scaled_norm(
        jnp.dot(normed, kv_down, preferred_element_type=jnp.float32), kv_gain
    ).astype(jnp.bfloat16)
    key_rot = rotate(
        jnp.dot(normed, rope_down, preferred_element_type=jnp.float32), own_position
    ).astype(jnp.bfloat16)
    packed = jnp.concatenate(
        [
            kv_lat,
            jnp.zeros((rows, NOPE), jnp.bfloat16),
            key_rot,
            jnp.zeros((rows, 128 - NOPE - ROPE), jnp.bfloat16),
        ],
        axis=1,
    )
    q_lat = scaled_norm(jnp.dot(normed, q_down, preferred_element_type=jnp.float32), q_gain).astype(
        jnp.bfloat16
    )
    swap = [(place, sp_count - 1 - place) for place in range(sp_count)]
    latents, q_group = gather(packed, q_lat)
    mate = sp_count - 1 - sp_place
    base = jnp.stack([sp_place * group_rows, mate * group_rows + half])
    position = (
        base[:, None, None]
        + (jnp.arange(tp_count) * rows)[None, :, None]
        + jnp.arange(half)[None, None, :]
    ).reshape(group_rows)
    angles = angle_tables(position).T

    q_up_turned = q_up.reshape(-1, heads, NOPE + ROPE).transpose(1, 2, 0)
    v_up = kv_up.reshape(rank, heads, HEAD_KV)[:, :, NOPE:].transpose(1, 2, 0)
    attended = attend(
        jnp.stack([sp_place, mate]).astype(jnp.int32),
        q_group,
        q_up_turned,
        jnp.cos(angles),
        jnp.sin(angles),
        position.astype(jnp.int32)[None, :],
        latents,
        kv_up,
        v_up.reshape(heads * VDIM, rank),
        rows,
    )
    own_heads = lax.all_to_all(
        attended.reshape(2, tp_count, half, heads * VDIM),
        "tp",
        split_axis=1,
        concat_axis=3,
        tiled=True,
    )
    returned = lax.ppermute(own_heads[1, 0], "sp", swap)
    own_rows = jnp.concatenate([own_heads[0, 0], returned], axis=0)
    projected = jnp.dot(own_rows, out_weight, preferred_element_type=jnp.float32)
    return scaled_norm(projected, out_gain).astype(jnp.bfloat16)


def solution(mesh):
    return jax.shard_map(
        local,
        mesh=mesh,
        in_specs=(
            P(("sp", "tp"), None),
            P(),
            P(),
            P(),
            P(),
            P(),
            P(),
            P(None, "tp"),
            P(None, "tp"),
            P(),
            P(),
        ),
        out_specs=P(("sp", "tp"), None),
        check_vma=False,
    )
```

```python
import functools

import jax
import jax.numpy as jnp
from jax import lax
from jax.experimental import pallas as pl
from jax.experimental.pallas import tpu as pltpu
from jax.sharding import PartitionSpec as P

NOPE = 64
ROPE = 32
VDIM = 64
HEAD_KV = NOPE + VDIM

EPS = 1e-06
THETA = 500000.0
LOG2E = 1.4426950408889634
FLOOR = -1e30
Q_TILE = 512
K_TILE = 512
V_ROWS = VDIM + 16


def scaled_norm(values_in, gain):
    values_in = values_in.astype(jnp.float32)
    return (
        values_in * lax.rsqrt(jnp.mean(values_in * values_in, axis=-1, keepdims=True) + EPS) * gain
    )


def angle_tables(position):
    inverse = 1.0 / THETA ** (jnp.arange(0, ROPE, 2, dtype=jnp.float32) / ROPE)
    return position.astype(jnp.float32)[:, None] * inverse[None, :]


def rotate(values_in, position):
    angles = angle_tables(position)
    cosine = jnp.cos(angles)
    sine = jnp.sin(angles)
    left = values_in[:, : ROPE // 2]
    right = values_in[:, ROPE // 2 :]
    return jnp.concatenate([left * cosine - right * sine, right * cosine + left * sine], axis=-1)


def attend_kernel(
    rows,
    heads,
    group_rows,
    rank,
    place_ref,
    q_lat_ref,
    q_up_ref,
    cos_ref,
    sin_ref,
    position_ref,
    lat_ref,
    turned_ref,
    kv_up_ref,
    v_up_ref,
    out_ref,
    query_ref,
    key_ref,
    value_ref,
    sum_ref,
    top_ref,
):
    chunk = pl.program_id(0)
    half = rows // 2
    side = group_rows // 2
    width = NOPE + ROPE
    scale = width**-0.5 * LOG2E

    @pl.when(chunk == 0)
    def _():
        cosine = cos_ref[...]
        sine = sin_ref[...]
        middle = NOPE + ROPE // 2
        for head in range(heads):
            turned = lax.dot_general(
                q_up_ref[head],
                q_lat_ref[...],
                (((1,), (1,)), ((), ())),
                preferred_element_type=jnp.float32,
            )
            left = turned[NOPE:middle]
            right = turned[middle:]
            query_ref[head, :NOPE] = turned[:NOPE].astype(jnp.bfloat16)
            query_ref[head, NOPE:middle] = (left * cosine - right * sine).astype(jnp.bfloat16)
            query_ref[head, middle:width] = (right * cosine + left * sine).astype(jnp.bfloat16)
            query_ref[head, width:] = jnp.zeros((128 - width, group_rows), jnp.bfloat16)
            row = lax.broadcasted_iota(jnp.int32, (16, group_rows), 0)
            value_ref[head, VDIM:] = jnp.where(row == 0, 1.0, 0.0).astype(jnp.bfloat16)
            sum_ref[head] = jnp.zeros((V_ROWS, group_rows), jnp.float32)
            top_ref[head] = jnp.full((1, group_rows), FLOOR, jnp.float32)

    own = place_ref[0]
    mate = place_ref[1]

    @pl.when(chunk <= jnp.maximum(own, mate))
    def _():
        lat = lat_ref[...].reshape(group_rows, rank)
        turned = turned_ref[...]
        lane = lax.broadcasted_iota(jnp.int32, (group_rows, HEAD_KV), 1)
        for head in range(heads):
            raw = jnp.dot(
                lat,
                kv_up_ref[:, head * HEAD_KV : (head + 1) * HEAD_KV],
                preferred_element_type=jnp.float32,
            ).astype(jnp.bfloat16)
            key_ref[head] = jnp.where(lane < NOPE, raw, turned)
        values = lax.dot_general(
            v_up_ref[...], lat, (((1,), (1,)), ((), ())), preferred_element_type=jnp.float32
        ).astype(jnp.bfloat16)
        for head in range(heads):
            value_ref[head, :VDIM] = values[head * VDIM : (head + 1) * VDIM]

        key_steps = group_rows // K_TILE
        query_steps = group_rows // Q_TILE

        def pair(masked, column, key_row):
            columns = pl.ds(column, Q_TILE)
            keys = pl.ds(key_row, K_TILE)
            if masked:
                key_index = (
                    chunk * group_rows
                    + key_row
                    + lax.broadcasted_iota(jnp.int32, (K_TILE, Q_TILE), 0)
                )
                visible = key_index <= position_ref[:, columns]
            every = range(heads)
            old = [top_ref[head, :, columns] for head in every]
            before = [sum_ref[head, :, columns] for head in every]
            new = []
            after = []
            for head in every:
                scores = jnp.dot(
                    key_ref[head, keys, :],
                    query_ref[head, :, columns],
                    preferred_element_type=jnp.float32,
                )
                if masked:
                    scores = jnp.where(visible, scores, FLOOR)
                top = jnp.maximum(old[head], jnp.max(scores, axis=0, keepdims=True))
                weights = jnp.exp2((scores - top) * scale)
                product = jnp.dot(
                    value_ref[head, :, keys],
                    weights.astype(jnp.bfloat16),
                    preferred_element_type=jnp.float32,
                )
                new.append(top)
                after.append(before[head] * jnp.exp2((old[head] - top) * scale) + product)
            for head in every:
                sum_ref[head, :, columns] = after[head]
                top_ref[head, :, columns] = new[head]

        @pl.loop(0, key_steps * query_steps)
        def _(index):
            column = pl.multiple_of(lax.rem(index, query_steps) * Q_TILE, Q_TILE)
            key_row = pl.multiple_of(lax.div(index, query_steps) * K_TILE, K_TILE)
            second = column >= side
            group = jnp.where(second, mate, own)
            inside = column - jnp.where(second, side, 0)
            base = group * group_rows + jnp.where(second, half, 0)
            first_query = base + lax.div(inside, half) * rows + lax.rem(inside, half)
            last = inside + Q_TILE - 1
            last_query = base + lax.div(last, half) * rows + lax.rem(last, half)
            first_key = chunk * group_rows + key_row
            last_key = first_key + K_TILE - 1

            @pl.when(last_key <= first_query)
            def _():
                pair(False, column, key_row)

            @pl.when((last_key > first_query) & (first_key <= last_query))
            def _():
                pair(True, column, key_row)

    @pl.when(chunk == pl.num_programs(0) - 1)
    def _():
        for column in range(0, group_rows, Q_TILE):
            columns = slice(column, column + Q_TILE)
            parts = [
                sum_ref[head, :VDIM, columns] / sum_ref[head, VDIM : VDIM + 1, columns]
                for head in range(heads)
            ]
            out_ref[columns, :] = jnp.concatenate(parts, axis=0).T.astype(jnp.bfloat16)


def attend(place, q_lat, q_up, cosine, sine, position, latents, turned, kv_up, v_up, rows):
    group_rows, q_rank = q_lat.shape
    heads = q_up.shape[0]
    rank = kv_up.shape[0]
    chunks = turned.shape[0] // group_rows
    tp_count = group_rows // rows

    def whole(*shape):
        return pl.BlockSpec(shape, lambda chunk, place_ref: (0,) * len(shape))

    pairs = turned.shape[0] * group_rows * heads // 2
    return pl.pallas_call(
        functools.partial(attend_kernel, rows, heads, group_rows, rank),
        out_shape=jax.ShapeDtypeStruct((group_rows, heads * VDIM), jnp.bfloat16),
        grid_spec=pltpu.PrefetchScalarGridSpec(
            num_scalar_prefetch=1,
            grid=(chunks,),
            in_specs=[
                whole(group_rows, q_rank),
                whole(heads, NOPE + ROPE, q_rank),
                whole(ROPE // 2, group_rows),
                whole(ROPE // 2, group_rows),
                whole(1, group_rows),
                pl.BlockSpec(
                    (tp_count, rows, rank),
                    lambda chunk, place_ref: (
                        jnp.minimum(chunk, jnp.maximum(place_ref[0], place_ref[1])),
                        0,
                        0,
                    ),
                ),
                pl.BlockSpec((group_rows, HEAD_KV), lambda chunk, place_ref: (chunk, 0)),
                whole(*kv_up.shape),
                whole(*v_up.shape),
            ],
            out_specs=whole(group_rows, heads * VDIM),
            scratch_shapes=[
                pltpu.VMEM((heads, 128, group_rows), jnp.bfloat16),
                pltpu.VMEM((heads, group_rows, HEAD_KV), jnp.bfloat16),
                pltpu.VMEM((heads, V_ROWS, group_rows), jnp.bfloat16),
                pltpu.VMEM((heads, V_ROWS, group_rows), jnp.float32),
                pltpu.VMEM((heads, 1, group_rows), jnp.float32),
            ],
        ),
        compiler_params=pltpu.CompilerParams(
            dimension_semantics=("arbitrary",), vmem_limit_bytes=48 * 1024 * 1024
        ),
        cost_estimate=pl.CostEstimate(
            flops=pairs * 640, bytes_accessed=latents.size * 2, transcendentals=pairs
        ),
    )(place, q_lat, q_up, cosine, sine, position, latents, turned, kv_up, v_up)


def plane_place(x, y, x_count, y_count):
    down = y_count - 1 - y
    across = jnp.where(lax.rem(down, 2) == 0, x - 1, x_count - 1 - x)
    return jnp.where(x == 0, y, y_count + down * (x_count - 1) + across)


def plane_chip(place, x_count, y_count):
    rest = jnp.maximum(place - y_count, 0)
    down = lax.div(rest, x_count - 1)
    step = lax.rem(rest, x_count - 1)
    across = jnp.where(lax.rem(down, 2) == 0, 1 + step, x_count - 1 - step)
    first = place < y_count
    return jnp.where(first, 0, across), jnp.where(first, place, y_count - 1 - down)


def ring_offsets(count):
    order = [0]
    for distance in range(1, count // 2 + 1):
        order.append(distance)
        if distance < count - distance:
            order.append(-distance)
    return order


def gather_kernel(
    sp_count, tp_count, lat_ref, q_ref, all_ref, q_all_ref, send_sem, recv_sem, q_send, q_recv, own_sem
):
    half = q_ref.shape[0] // 2
    extra = lat_ref.shape[0] - 2 * half
    starts, sizes = (0, half + extra), (half + extra, half)
    y_count = tp_count // 2
    x_count = y_count
    z_count = sp_count // x_count
    plane_count = x_count * y_count
    sp = lax.axis_index("sp")
    tp = lax.axis_index("tp")
    z, x = lax.div(sp, x_count), lax.rem(sp, x_count)
    y, core = lax.div(tp, 2), lax.rem(tp, 2)
    plane = plane_place(x, y, x_count, y_count)
    mate = sp_count - 1 - sp

    def device(z_at, plane_at, core_at):
        x_at, y_at = plane_chip(plane_at, x_count, y_count)
        return z_at * x_count + x_at, y_at * 2 + core_at

    def wrap(value, count):
        return lax.rem(value + count, count)

    z_up, z_down = wrap(z + 1, z_count), wrap(z - 1, z_count)
    p_up, p_down = wrap(plane + 1, plane_count), wrap(plane - 1, plane_count)
    neighbours = [
        device(z_up, plane, core),
        device(z_down, plane, core),
        device(z, p_up, core),
        device(z, p_down, core),
    ]
    others = [wrap(tp + step, tp_count) for step in range(1, tp_count)]
    greeted = neighbours + [(sp, other) for other in others]
    greeted += [(mate, tp)]
    barrier = pltpu.get_barrier_semaphore()
    for target in greeted:
        pl.semaphore_signal(
            barrier, inc=1, device_id=target, device_id_type=pl.DeviceIdType.MESH
        )
    pl.semaphore_wait(barrier, len(greeted))

    own_slot = sp * tp_count + tp
    own_copies = [
        pltpu.make_async_copy(lat_ref, all_ref.at[own_slot], own_sem.at[0]),
        pltpu.make_async_copy(q_ref.at[pl.ds(0, half)], q_all_ref.at[0, tp], own_sem.at[1]),
    ]
    for copy in own_copies:
        copy.start()

    sames = [wrap(tp + 2 * step, tp_count) for step in range(1, y_count)]
    partner_tp = y * 2 + 1 - core

    def q_copy(side, source, target, index, mine):
        landed = q_all_ref.at[side, source]
        return pltpu.make_async_remote_copy(
            src_ref=q_ref.at[pl.ds(side * half, half)] if mine else landed,
            dst_ref=landed,
            send_sem=q_send.at[index],
            recv_sem=q_recv.at[side, source],
            device_id=target,
            device_id_type=pl.DeviceIdType.MESH,
        )

    q_copies = []

    def q_push(side, source, target, mine):
        copy = q_copy(side, source, target, len(q_copies), mine)
        copy.start()
        q_copies.append(copy)

    q_push(1, tp, (mate, tp), True)
    for same in sames:
        q_push(0, tp, (sp, same), True)
    q_push(0, tp, (sp, partner_tp), True)
    q_first = tuple(q_copies)

    def finish_q():
        del q_copies[len(q_first) :]
        q_copy(1, tp, (mate, tp), 0, False).wait_recv()
        for same in sames:
            q_push(1, tp, (sp, same), False)
        q_push(1, tp, (sp, partner_tp), False)
        for side in range(2):
            for same in sames:
                q_copy(side, same, (mate, tp), 0, False).wait_recv()
                q_push(side, same, (sp, partner_tp), False)
        for side in range(2):
            for at in range(y_count):
                q_copy(side, at * 2 + 1 - core, (mate, tp), 0, False).wait_recv()
        for copy in q_copies:
            copy.wait_send()

    def when(condition, action):
        if condition is None:
            action()
        else:
            pl.when(condition)(action)

    def both(left, right):
        if left is None or right is None:
            return right if left is None else left
        return left & right

    def ring_sends(offset, piece, count, at, line):
        ways = []
        if line:
            if offset >= 0:
                ways.append((0, at + 1 < count))
            if offset <= 0:
                ways.append((1, at > 0))
            return ways
        far = count // 2
        if offset <= 0 and offset != far:
            distance = 1 - offset
            if distance < far or (distance == far and piece == 1):
                ways.append((1, None))
        if offset >= 0 and offset != far:
            distance = 1 + offset
            if distance < far or (distance == far and piece == 0):
                ways.append((0, None))
        return ways

    def offsets_of(count, line):
        if not line:
            return ring_offsets(count)
        return [0] + [sign * step for step in range(1, count) for sign in (1, -1)]

    def exists(offset, count, at, line):
        if not line or offset == 0:
            return None
        return at >= offset if offset > 0 else at - offset < count

    def spread(core_at, count_1, count_2, at_1, at_2, line_1, line_2, place):
        sent = []

        def part(slot, piece):
            return all_ref.at[slot, pl.ds(starts[piece], sizes[piece])]

        def slot_of(one, two, core_of):
            sp_of, tp_of = device(*place(one, two), core_of)
            return sp_of * tp_count + tp_of

        def push(slot, piece, target, mine, condition):
            source = (
                lat_ref.at[pl.ds(starts[piece], sizes[piece])] if mine else part(slot, piece)
            )
            copy = pltpu.make_async_remote_copy(
                src_ref=source,
                dst_ref=part(slot, piece),
                send_sem=send_sem.at[len(sent)],
                recv_sem=recv_sem.at[slot, piece],
                device_id=target,
                device_id_type=pl.DeviceIdType.MESH,
            )
            when(condition, copy.start)
            sent.append((copy, condition))

        def arrive(slot, piece, condition):
            copy = pltpu.make_async_remote_copy(
                src_ref=part(slot, piece),
                dst_ref=part(slot, piece),
                send_sem=send_sem.at[0],
                recv_sem=recv_sem.at[slot, piece],
                device_id=neighbours[0],
                device_id_type=pl.DeviceIdType.MESH,
            )
            when(condition, copy.wait_recv)

        ways_1 = [
            device(*place(wrap(at_1 + step, count_1), at_2), core_at) for step in (1, -1)
        ]
        ways_2 = [
            device(*place(at_1, wrap(at_2 + step, count_2)), core_at) for step in (1, -1)
        ]
        partner = (sp, y * 2 + 1 - core_at)
        items = [
            (one, two)
            for one in offsets_of(count_1, line_1)
            for two in offsets_of(count_2, line_2)
        ]
        items.sort(key=lambda item: (abs(item[0]) + abs(item[1]), abs(item[1])))
        swapped = []
        for one, two in items:
            slot = slot_of(wrap(at_1 - one, count_1), wrap(at_2 - two, count_2), core_at)
            mine = one == 0 and two == 0
            here = both(exists(one, count_1, at_1, line_1), exists(two, count_2, at_2, line_2))
            for piece in range(2):
                if not mine:
                    arrive(slot, piece, here)
                if two == 0:
                    for way, condition in ring_sends(one, piece, count_1, at_1, line_1):
                        push(slot, piece, ways_1[way], mine, both(here, condition))
                for way, condition in ring_sends(two, piece, count_2, at_2, line_2):
                    push(slot, piece, ways_2[way], mine, both(here, condition))
                push(slot, piece, partner, mine, here)
        finish_q()
        for z_from in range(z_count):
            for plane_from in range(plane_count):
                sp_of, tp_of = device(z_from, plane_from, 1 - core_at)
                for piece in range(2):
                    arrive(sp_of * tp_count + tp_of, piece, None)
        for copy, condition in sent:
            when(condition, copy.wait_send)

    @pl.when(core == 0)
    def _():
        spread(0, plane_count, z_count, plane, z, False, True, lambda one, two: (two, one))

    @pl.when(core == 1)
    def _():
        spread(1, z_count, plane_count, z, plane, True, False, lambda one, two: (one, two))

    for copy in own_copies:
        copy.wait()


def gather(latents, q_lat):
    sp_count = lax.axis_size("sp")
    tp_count = lax.axis_size("tp")
    rows, width = latents.shape
    count = sp_count * tp_count
    space = pl.BlockSpec(memory_space=pltpu.VMEM)
    everywhere, q_all = pl.pallas_call(
        functools.partial(gather_kernel, sp_count, tp_count),
        out_shape=(
            jax.ShapeDtypeStruct((count, rows, width), latents.dtype),
            jax.ShapeDtypeStruct((2, tp_count, q_lat.shape[0] // 2, q_lat.shape[1]), q_lat.dtype),
        ),
        in_specs=[space, space],
        out_specs=(pl.BlockSpec(memory_space=pl.ANY), pl.BlockSpec(memory_space=pl.ANY)),
        scratch_shapes=[
            pltpu.SemaphoreType.DMA((5 * count,)),
            pltpu.SemaphoreType.DMA((count, 2)),
            pltpu.SemaphoreType.DMA((3 * tp_count,)),
            pltpu.SemaphoreType.DMA((2, tp_count)),
            pltpu.SemaphoreType.DMA((2,)),
        ],
        compiler_params=pltpu.CompilerParams(collective_id=0, has_side_effects=True),
        cost_estimate=pl.CostEstimate(
            flops=0, bytes_accessed=count * rows * width * 8, transcendentals=0
        ),
    )(latents, q_lat)
    return everywhere, q_all.reshape(tp_count * q_lat.shape[0], -1)


def deliver_kernel(sp_count, tp_count, in_ref, out_ref, send_sem, recv_sem, own_sem):
    half = out_ref.shape[0] // 2
    width = in_ref.shape[1]
    sp = lax.axis_index("sp")
    tp = lax.axis_index("tp")
    mate = sp_count - 1 - sp
    targets = [(0, sp, lax.rem(tp + step, tp_count)) for step in range(1, tp_count)]
    targets = [(1, mate, lax.rem(tp + step, tp_count)) for step in range(tp_count)] + targets
    barrier = pltpu.get_barrier_semaphore()
    for _, group, place in targets:
        pl.semaphore_signal(
            barrier, inc=1, device_id=(group, place), device_id_type=pl.DeviceIdType.MESH
        )
    pl.semaphore_wait(barrier, len(targets))
    columns = pl.ds(pl.multiple_of(tp * width, width), width)

    def source(side, place):
        first = pl.multiple_of((side * tp_count + place) * half, half)
        return in_ref.at[pl.ds(first, half)]

    copies = []
    for index, (side, group, place) in enumerate(targets):
        copy = pltpu.make_async_remote_copy(
            src_ref=source(side, place),
            dst_ref=out_ref.at[pl.ds(side * half, half), columns],
            send_sem=send_sem.at[index],
            recv_sem=recv_sem.at[side, tp],
            device_id=(group, place),
            device_id_type=pl.DeviceIdType.MESH,
        )
        copy.start()
        copies.append(copy)
    own = pltpu.make_async_copy(source(0, tp), out_ref.at[pl.ds(0, half), columns], own_sem)
    own.start()
    for side, _, place in targets:
        landed = out_ref.at[
            pl.ds(side * half, half), pl.ds(pl.multiple_of(place * width, width), width)
        ]
        pltpu.make_async_remote_copy(
            src_ref=landed,
            dst_ref=landed,
            send_sem=send_sem.at[0],
            recv_sem=recv_sem.at[side, place],
            device_id=(mate, tp),
            device_id_type=pl.DeviceIdType.MESH,
        ).wait_recv()
    own.wait()
    for copy in copies:
        copy.wait_send()


def deliver(attended):
    sp_count = lax.axis_size("sp")
    tp_count = lax.axis_size("tp")
    group_rows, width = attended.shape
    space = pl.BlockSpec(memory_space=pltpu.VMEM)
    return pl.pallas_call(
        functools.partial(deliver_kernel, sp_count, tp_count),
        out_shape=jax.ShapeDtypeStruct(
            (group_rows // tp_count, tp_count * width), attended.dtype
        ),
        in_specs=[space],
        out_specs=space,
        scratch_shapes=[
            pltpu.SemaphoreType.DMA((2 * tp_count,)),
            pltpu.SemaphoreType.DMA((2, tp_count)),
            pltpu.SemaphoreType.DMA,
        ],
        compiler_params=pltpu.CompilerParams(collective_id=1, has_side_effects=True),
    )(attended)


def local(
    tokens,
    norm_gain,
    q_down,
    kv_down,
    rope_down,
    q_gain,
    kv_gain,
    q_up,
    kv_up,
    out_weight,
    out_gain,
):
    rows = tokens.shape[0]
    tp_count = lax.axis_size("tp")
    sp_count = lax.axis_size("sp")
    tp_place = lax.axis_index("tp")
    sp_place = lax.axis_index("sp")
    group_rows = rows * tp_count
    half = rows // 2
    row_first = (sp_place * tp_count + tp_place) * rows
    own_position = row_first + jnp.arange(rows)
    heads = q_up.shape[1] // (NOPE + ROPE)
    rank = kv_up.shape[0]

    normed = scaled_norm(tokens, norm_gain).astype(jnp.bfloat16)
    kv_lat = scaled_norm(
        jnp.dot(normed, kv_down, preferred_element_type=jnp.float32), kv_gain
    ).astype(jnp.bfloat16)
    key_rot = rotate(
        jnp.dot(normed, rope_down, preferred_element_type=jnp.float32), own_position
    ).astype(jnp.bfloat16)
    rot_rows = rows * ROPE // rank
    extra = -(-rot_rows // 16) * 16
    packed = jnp.concatenate(
        [
            kv_lat,
            key_rot.reshape(rot_rows, rank),
            jnp.zeros((extra - rot_rows, rank), jnp.bfloat16),
        ],
        axis=0,
    )
    q_lat = scaled_norm(jnp.dot(normed, q_down, preferred_element_type=jnp.float32), q_gain).astype(
        jnp.bfloat16
    )
    latents, q_group = gather(packed, q_lat)
    turned = latents[:, rows : rows + rot_rows].reshape(-1, ROPE)
    turned = jnp.pad(turned, ((0, 0), (NOPE, HEAD_KV - NOPE - ROPE)))
    mate = sp_count - 1 - sp_place
    base = jnp.stack([sp_place * group_rows, mate * group_rows + half])
    position = (
        base[:, None, None]
        + (jnp.arange(tp_count) * rows)[None, :, None]
        + jnp.arange(half)[None, None, :]
    ).reshape(group_rows)
    angles = angle_tables(position).T

    q_up_turned = q_up.reshape(-1, heads, NOPE + ROPE).transpose(1, 2, 0)
    v_up = kv_up.reshape(rank, heads, HEAD_KV)[:, :, NOPE:].transpose(1, 2, 0)
    attended = attend(
        jnp.stack([sp_place, mate]).astype(jnp.int32),
        q_group,
        q_up_turned,
        jnp.cos(angles),
        jnp.sin(angles),
        position.astype(jnp.int32)[None, :],
        latents,
        turned,
        kv_up,
        v_up.reshape(heads * VDIM, rank),
        rows,
    )
    own_rows = deliver(attended)
    projected = jnp.dot(own_rows, out_weight, preferred_element_type=jnp.float32)
    return scaled_norm(projected, out_gain).astype(jnp.bfloat16)


def solution(mesh):
    return jax.shard_map(
        local,
        mesh=mesh,
        in_specs=(
            P(("sp", "tp"), None),
            P(),
            P(),
            P(),
            P(),
            P(),
            P(),
            P(None, "tp"),
            P(None, "tp"),
            P(),
            P(),
        ),
        out_specs=P(("sp", "tp"), None),
        check_vma=False,
    )
```
